768 devices in a mesh: row: 48 (over z, x), col: 16 (over y, core).
Axes of the slice: x: 4, y: 8, z: 12, core: 2. Of those that a mesh axis runs over, the one named last changes fastest.
Arguments:
- tokens: bfloat16 [6144, 4096], P('row'), may hold values from -6 to 6
- w_value: bfloat16 [2304, 4096], P('col'), may hold values from -0.09375 to 0.09375
- w_gate_one: bfloat16 [2304, 4096], P('col'), may hold values from -0.09375 to 0.09375
- w_gate_two: bfloat16 [2304, 4096], P('col'), may hold values from -0.09375 to 0.09375
- short_taps: float32 [3, 3, 2304], P(None, None, 'col'), may hold values from -3.5 to 3.5
- filter_in: float32 [33, 64], replicated, may hold values from -1 to 1
- filter_mid: float32 [64, 64], replicated, may hold values from -0.75 to 0.75
- filter_out: float32 [64, 2, 2, 2304], replicated, may hold values from -1 to 1
- decay_rate: float32 [2304], P('col'), may hold values from 0.5 to 49, as said below
- skip: float32 [2, 2304], P(None, 'col'), may hold values from -0.3 to 0.3
- w_out: bfloat16 [2304, 4096], P(None, 'col'), may hold values from -0.125 to 0.125
Outputs:
- mixed: bfloat16 [6144, 4096], P('row', 'col')
The draws below stay inside these ranges and needn't reach their ends.
Inputs may be any that keep to these rules, and one draw needn't show every extreme that they name: `decay_rate`: each channel's rate is positive; per unit of the relative position t.
All inputs are finite; a program needn't handle non-finite values.
Results may differ from the reference program's by a relative error of at most 0.007.
Values may be sent and summed in bfloat16 or wider, within the bound.
A program may use at most 32 MiB of HBM per device.

```python
import math
import jax
import jax.numpy as jnp
from jax import lax

D = 4096
HW = 2304
FILTER_HID = 64
BANDS = 16
EMB = 33
SEQ = 6144


def channel_rates(key, fast_share):
    key_slow, key_fast, key_pick = jax.random.split(jax.random.fold_in(key, 11), 3)
    slow_rates = jnp.exp(jax.random.uniform(key_slow, (HW,), jnp.float32, math.log(0.5), math.log(2.0)))
    fast_rates = jnp.exp(jax.random.uniform(key_fast, (HW,), jnp.float32, math.log(SEQ / 154.0), math.log(SEQ / 128.0)))
    chosen = jax.random.uniform(key_pick, (HW,), jnp.float32) < fast_share
    return jnp.where(chosen, fast_rates, slow_rates)


def draw_decay_rate(key, part):
    fast_share = 0.5
    return channel_rates(key, fast_share)


def draw_filter_out(key, part):
    fast_share = 0.5
    rates = channel_rates(key, fast_share)
    column_scale = jnp.sqrt(2.0 * rates / (1.0 - jnp.exp(-2.0 * rates)))
    noise = jax.random.truncated_normal(jax.random.fold_in(key, 23), -4.0, 4.0, (FILTER_HID, 2, 2, HW), jnp.float32)
    return noise * column_scale / math.sqrt(FILTER_HID * SEQ)


def steps_of(own_key, shape, cuts, least, largest):
    def one(position, blocks):
        heights = jax.random.uniform(jax.random.fold_in(jax.random.fold_in(own_key, 6), position), (blocks,), jnp.float32, least / len(cuts), largest / len(cuts))
        return jnp.repeat(jnp.exp(heights), shape[position] // blocks).reshape((-1,) + (1,) * (len(shape) - position - 1))

    loudness = one(*cuts[0])
    for cut in cuts[1:]:
        loudness = loudness * one(*cut)
    return loudness


def gaussian(own_key, extent, width, most, pieces=(), kind=jnp.bfloat16):
    array = jax.random.normal(own_key, extent, jnp.float32) * width
    if len(pieces) > 0:
        array = steps_of(own_key, extent, pieces, -0.22, 0.18) * array
    return jnp.clip(array, min=-most, max=most).astype(kind)


def setup_inputs(seed: int = 0) -> dict:
    splits = jax.random.split(jax.random.key(seed), 12)
    return {
        "tokens": gaussian(splits[0], (SEQ, D), 1.0, 6.0, ((0, 48),)),
        "w_value": gaussian(splits[1], (HW, D), D ** -0.5, 0.09375, ((0, 16),)),
        "w_gate_one": gaussian(splits[2], (HW, D), D ** -0.5, 0.09375, ((0, 16),)),
        "w_gate_two": gaussian(splits[3], (HW, D), D ** -0.5, 0.09375, ((0, 16),)),
        "short_taps": gaussian(splits[4], (3, 3, HW), 3 ** -0.5, 3.5, ((2, 16),), jnp.float32),
        "filter_in": jnp.clip(jax.random.uniform(splits[5], (EMB, FILTER_HID), jnp.float32, -1.0, 1.0), -1.0, 1.0),
        "filter_mid": jnp.clip(jax.random.uniform(splits[6], (FILTER_HID, FILTER_HID), jnp.float32, -0.75, 0.75), -0.75, 0.75),
        "filter_out": draw_filter_out(jax.random.fold_in(splits[11], 71), 0),
        "decay_rate": draw_decay_rate(jax.random.fold_in(splits[11], 71), 0),
        "skip": jnp.clip(jax.random.uniform(splits[9], (2, HW), jnp.float32, -0.3, 0.3) * steps_of(splits[9], (2, HW), ((1, 16),), -0.4, 0.0), -0.3, 0.3),
        "w_out": gaussian(splits[10], (HW, D), HW ** -0.5, 0.125, ((1, 16),)),
    }


HIGHEST = lax.Precision.HIGHEST


def filter_bank(filter_in, filter_mid, out_block, rate_block):
    positions = jnp.arange(SEQ, dtype=jnp.float32)
    relative = positions / (SEQ - 1)
    bands = jnp.linspace(1e-4, BANDS - 1, BANDS, dtype=jnp.float32)
    angles = (2 * math.pi / SEQ) * positions[:, None] * bands[None, :]
    feats = jnp.concatenate([relative[:, None], jnp.cos(angles), jnp.sin(angles)], axis=1)
    hidden = jnp.sin(jnp.dot(feats, filter_in, precision=HIGHEST))
    hidden = jnp.sin(jnp.dot(hidden, filter_mid, precision=HIGHEST))
    filter_taps = jnp.einsum('lh,hodc->odcl', hidden, out_block, precision=HIGHEST)
    decay = jnp.exp(-relative[None, :] * rate_block[:, None])
    return filter_taps * decay


def reference(tokens, w_value, w_gate_one, w_gate_two, short_taps, filter_in, filter_mid, filter_out, decay_rate, skip, w_out):
    projected = jnp.stack([jnp.dot(tokens, weight.T, preferred_element_type=jnp.float32).astype(jnp.bfloat16)
                           for weight in (w_value, w_gate_one, w_gate_two)])
    projected = lax.optimization_barrier(projected).astype(jnp.float32)
    padded = jnp.pad(projected, ((0, 0), (1, 1), (0, 0)))
    shorted = (padded[:, :-2] * short_taps[:, 0][:, None, :] + padded[:, 1:-1] * short_taps[:, 1][:, None, :]
               + padded[:, 2:] * short_taps[:, 2][:, None, :])
    n_blocks = HW // 128
    inputs = shorted.reshape(3, SEQ, n_blocks, 128).transpose(2, 0, 3, 1)
    out_blocks = filter_out.reshape(FILTER_HID, 2, 2, n_blocks, 128).transpose(3, 0, 1, 2, 4)
    rate_blocks = decay_rate.reshape(n_blocks, 128)
    skip_blocks = skip.reshape(2, n_blocks, 128).transpose(1, 0, 2)

    def mix_block(packed):
        block_in, out_block, rate_block, skip_block = packed
        filter_taps = filter_bank(filter_in, filter_mid, out_block, rate_block)
        forward_part = filter_taps[:, 0]
        backward_part = filter_taps[:, 1]
        kern = jnp.concatenate([forward_part, jnp.zeros(forward_part[..., :1].shape, jnp.float32),
                                backward_part[..., 1:][..., ::-1]], axis=-1)
        spectrum = jnp.fft.rfft(kern, axis=-1)
        signal = block_in[0]
        for order_index in range(2):
            signal_freq = jnp.fft.rfft(signal, n=2 * SEQ, axis=-1)
            long_part = jnp.fft.irfft(signal_freq * spectrum[order_index], n=2 * SEQ, axis=-1)[..., :SEQ]
            signal = block_in[order_index + 1] * (long_part + skip_block[order_index][:, None] * signal)
        return signal.astype(jnp.bfloat16)

    outputs = lax.map(mix_block, (inputs, out_blocks, rate_blocks, skip_blocks))
    mixer_out = outputs.transpose(2, 0, 1).reshape(SEQ, HW)
    return jnp.dot(mixer_out, w_out, preferred_element_type=jnp.float32).astype(jnp.bfloat16)
```

```python
import functools
import math

import jax
import jax.numpy as jnp
import ml_dtypes
import numpy as np
from jax import lax
from jax.experimental import pallas as pl
from jax.experimental.pallas import tpu as pltpu
from jax.sharding import PartitionSpec as P

BANDS = 16
BLOCK = 128
CHUNK_BLOCKS = 4
SINE = (
    6.283185272722434,
    -41.34169706895579,
    81.60502462256538,
    -76.70155117606154,
    42.01616582018448,
    -14.868610989100207,
    3.199693650180954,
)
MESH = pl.DeviceIdType.MESH
F32 = jnp.float32
BF16 = jnp.bfloat16


def halves(table):
    high = table.astype(ml_dtypes.bfloat16)
    low = (table - high.astype(np.float64)).astype(ml_dtypes.bfloat16)
    return high, low


def constants(rows, seq_len):
    wide = 2 * rows
    total = wide * BLOCK
    odd = np.arange(rows)[:, None] + 0.5
    blocks = np.arange(rows)[None, :]
    one = 2 * np.pi * odd * blocks / wide
    first = np.concatenate([np.cos(one), -np.sin(one)], axis=0)
    last = np.concatenate([np.cos(one).T, -np.sin(one).T], axis=1) * (2.0 / total)
    first_h, first_l = halves(first)
    last_h, last_l = halves(last)
    first = np.concatenate([first_h, first_l, first_h], axis=1)
    last = np.concatenate([last_h, last_l, last_h], axis=1)
    lanes = np.arange(BLOCK)
    two = 2 * np.pi * odd * lanes[None, :] / total
    twiddle = np.stack([np.cos(two), np.sin(two)]).astype(np.float32)
    three = 2 * np.pi * (lanes[:, None] * lanes[None, :] % BLOCK) / BLOCK
    cosine, sine = np.cos(three), np.sin(three)
    forward = np.block([[cosine, -sine], [sine, cosine]])
    inverse = np.block([[cosine, sine], [-sine, cosine]])
    square = np.stack([*halves(forward), *halves(inverse)])
    chunk = CHUNK_BLOCKS * BLOCK
    bands = np.linspace(0.0001, BANDS - 1, BANDS, dtype=np.float32).astype(np.float64)
    rate = 2 * np.pi / seq_len * bands[:, None]
    inside = rate * np.arange(chunk)[None, :]
    base = np.concatenate([np.cos(inside), np.sin(inside)]).astype(np.float32)
    steps = np.arange(seq_len // chunk)[:, None, None] * chunk * rate[None]
    turn = np.concatenate([np.cos(steps), np.sin(steps)], axis=1)
    turn = np.broadcast_to(turn, turn.shape[:2] + (BLOCK,)).astype(np.float32)
    return first, last, twiddle, square, base, np.ascontiguousarray(turn)


def dot(left, right, dims=((1,), (0,))):
    return lax.dot_general(left, right, (dims, ((), ())), preferred_element_type=F32)


def split(value):
    high = value.astype(BF16)
    return high, (value - high.astype(F32)).astype(BF16)


def sine_of_turns(turns):
    part = turns - jnp.round(turns)
    square = part * part
    total = jnp.full_like(square, SINE[-1])
    for coefficient in SINE[-2::-1]:
        total = total * square + coefficient
    return total * part


def stacked(value):
    high, low = split(value)
    return jnp.concatenate([high, high, low], axis=0)


def tripled(weights, width):
    high = weights.astype(BF16).astype(F32)
    lane = lax.broadcasted_iota(jnp.int32, weights.shape, 1)
    middle = (lane >= width) & (lane < 2 * width)
    return jnp.where(middle, weights - high, high).astype(BF16)


def kernel(
    sizes,
    taps_s,
    skip_s,
    rate_s,
    tokens_h,
    value_h,
    gate_one_h,
    gate_two_h,
    out_h,
    params,
    first,
    last,
    twiddle,
    square,
    base,
    turn,
    result,
    tokens_v,
    weights_v,
    out_v,
    plain,
    spread,
    gathered_taps,
    spectra,
    send_v,
    send_g,
    recv_v,
    recv_g,
    send_y,
    recv_y,
    blocks,
    load_sem,
    send_sem,
    recv_sem,
    near_send,
    near_recv,
    pair_send,
    pair_recv,
):
    rows, cols, chan, early = sizes
    width = rows * chan
    chips = cols // 2
    row = lax.axis_index("row")
    col = lax.axis_index("col")
    place = col // 2
    core = col % 2
    partner = place * 2 + 1 - core

    loads = [
        pltpu.make_async_copy(tokens_h, tokens_v, load_sem.at[0]),
        pltpu.make_async_copy(value_h, weights_v.at[0], load_sem.at[1]),
        pltpu.make_async_copy(gate_one_h, weights_v.at[1], load_sem.at[2]),
        pltpu.make_async_copy(gate_two_h, weights_v.at[2], load_sem.at[3]),
        pltpu.make_async_copy(out_h, out_v, load_sem.at[4]),
    ]
    for load in loads:
        load.start()

    barrier = pltpu.get_barrier_semaphore()

    @pl.loop(1, rows)
    def _(step):
        other = lax.rem(row + step, rows)
        pl.semaphore_signal(barrier, inc=1, device_id=(other, col), device_id_type=MESH)

    @pl.loop(1, chips)
    def _(step):
        other = lax.rem(place + step, chips) * 2 + core
        pl.semaphore_signal(barrier, inc=1, device_id=(row, other), device_id_type=MESH)

    pl.semaphore_signal(barrier, inc=1, device_id=(row, partner), device_id_type=MESH)

    loads[0].wait()
    for which in range(3):
        loads[1 + which].wait()
        projected = dot(weights_v[which], tokens_v[...], ((1,), (1,)))
        plain[...] = projected.astype(BF16).astype(F32)
        stride, offset = (4, 0) if which == 0 else (8, (which - 1) * chan)
        for q in range(chan):
            spread[pl.ds(offset + q, rows, stride=stride), :] = plain[
                pl.ds(q, rows, stride=chan), :
            ]
        if which == 0:
            for q in range(chan, 4):
                spread[pl.ds(q, rows, stride=4), :] = jnp.zeros((rows, BLOCK), F32)
            for r in range(rows):
                send_v[r] = spread[4 * r : 4 * r + 4, :].astype(BF16)
    for q in range(2 * chan, 8):
        spread[pl.ds(q, rows, stride=8), :] = jnp.zeros((rows, BLOCK), F32)
    for r in range(rows):
        send_g[r] = spread[8 * r : 8 * r + 8, :].astype(BF16)

    n_chunks = rows // CHUNK_BLOCKS
    chunk = CHUNK_BLOCKS * BLOCK
    seq_len = rows * BLOCK
    in_w = tripled(params[0:64, 0:144], 48)
    mid_w = tripled(params[64:128, 0:192], 64)
    out_w = tripled(params[128:144, 0:192], 64)
    rate_rows = jnp.zeros((16, BLOCK), F32)
    channel = lax.rem(lax.broadcasted_iota(jnp.int32, (16, BLOCK), 0), chan)
    for q in range(chan):
        rate_rows = jnp.where(channel == q, rate_s[row * chan + q], rate_rows)
    rate_rows = jnp.concatenate([rate_rows] * CHUNK_BLOCKS, axis=1)

    def filter_chunk(index):
        lane = lax.broadcasted_iota(jnp.int32, (16, chunk), 1)
        relative = (lane + index * chunk).astype(F32) * (1.0 / (seq_len - 1))
        first_row = lax.broadcasted_iota(jnp.int32, (16, chunk), 0) == 0
        turn_c = jnp.concatenate([turn[index, 0:BANDS, :]] * CHUNK_BLOCKS, axis=1)
        turn_s = jnp.concatenate([turn[index, BANDS : 2 * BANDS, :]] * CHUNK_BLOCKS, axis=1)
        base_c, base_s = base[0:BANDS, :], base[BANDS : 2 * BANDS, :]
        feats = jnp.concatenate(
            [
                base_c * turn_c - base_s * turn_s,
                base_s * turn_c + base_c * turn_s,
                jnp.where(first_row, relative, 0.0),
            ],
            axis=0,
        )
        hidden = sine_of_turns(dot(in_w, stacked(feats)))
        hidden = sine_of_turns(dot(mid_w, stacked(hidden)))
        filter_taps = dot(out_w, stacked(hidden)) * jnp.exp(-relative * rate_rows)
        for b in range(CHUNK_BLOCKS):
            start = pl.multiple_of((index * CHUNK_BLOCKS + b) * 16, 16)
            gathered_taps[pl.ds(start, 16), :] = filter_taps[:, b * BLOCK : (b + 1) * BLOCK]

    @pl.loop(0, early)
    def _(index):
        filter_chunk(index)

    pl.semaphore_wait(barrier, rows - 1 + chips - 1 + 1)

    def send(source, landing, which, order):
        @pl.loop(0, rows - 1)
        def _(step):
            half = (step + 1) // 2
            sign = 1 - 2 * lax.rem(step, 2)
            other = lax.rem(row + rows // 2 + rows + sign * half, rows)
            pltpu.make_async_remote_copy(
                src_ref=source.at[other],
                dst_ref=landing.at[row],
                send_sem=send_sem.at[which],
                recv_sem=recv_sem.at[which],
                device_id=(other, col),
                device_id_type=MESH,
            ).start()

    def all_of(source, landing, which):
        return pltpu.make_async_remote_copy(
            src_ref=source.at[pl.ds(0, rows - 1)],
            dst_ref=landing.at[pl.ds(0, rows - 1)],
            send_sem=send_sem.at[which],
            recv_sem=recv_sem.at[which],
            device_id=(lax.rem(row + 1, rows), col),
            device_id_type=MESH,
        )

    send(send_v, recv_v, 0, 0)
    send(send_g, recv_g, 1, 0)
    recv_v[row] = send_v[row]
    recv_g[row] = send_g[row]

    @pl.loop(early, n_chunks)
    def _(index):
        filter_chunk(index)

    tw_c, tw_s = twiddle[0], twiddle[1]

    def forward(signals):
        reals, imags = [], []
        for signal in signals:
            both = dot(first[...], stacked(signal))
            re, im = both[:rows], both[rows:]
            reals.append(re * tw_c + im * tw_s)
            imags.append(im * tw_c - re * tw_s)
        both = jnp.concatenate(
            [jnp.concatenate(reals, axis=0), jnp.concatenate(imags, axis=0)], axis=1
        )
        high, low = split(both)
        return dot(high, square[0]) + dot(high, square[1]) + dot(low, square[0])

    def backward(spectrum):
        high, low = split(spectrum)
        both = dot(high, square[2]) + dot(high, square[3]) + dot(low, square[2])
        signals = []
        for q in range(chan):
            re = both[q * rows : (q + 1) * rows, :BLOCK]
            im = both[q * rows : (q + 1) * rows, BLOCK:]
            turned = jnp.concatenate([re * tw_c - im * tw_s, im * tw_c + re * tw_s], axis=0)
            signals.append(dot(last[...], stacked(turned)))
        return signals

    lane = lax.broadcasted_iota(jnp.int32, (rows, BLOCK), 1)
    line = lax.broadcasted_iota(jnp.int32, (rows, BLOCK), 0)
    origin = (lane == 0) & (line == 0)
    for order in range(2):
        ahead, behind = [], []
        for q in range(chan):
            base_row = (order * 2) * chan + q
            ahead.append(gathered_taps[pl.ds(base_row, rows, stride=16), :])
            back = gathered_taps[pl.ds(base_row + chan, rows, stride=16), :]
            behind.append(jnp.where(origin, 0.0, back))
        ahead = forward(ahead)
        behind = forward(behind)
        spectra[order, :, :BLOCK] = ahead[:, :BLOCK] + behind[:, :BLOCK]
        spectra[order, :, BLOCK:] = ahead[:, BLOCK:] - behind[:, BLOCK:]

    def short(signal, which, q):
        before = pltpu.roll(signal, 1, 1)
        before = jnp.where(lane == 0, pltpu.roll(before, 1, 0), before)
        before = jnp.where(origin, 0.0, before)
        after = pltpu.roll(signal, BLOCK - 1, 1)
        after = jnp.where(lane == BLOCK - 1, pltpu.roll(after, rows - 1, 0), after)
        after = jnp.where((lane == BLOCK - 1) & (line == rows - 1), 0.0, after)
        at = row * chan + q
        return (
            before * taps_s[which * 3, at]
            + signal * taps_s[which * 3 + 1, at]
            + after * taps_s[which * 3 + 2, at]
        )

    all_of(send_v, recv_v, 0).wait_recv()
    for r in range(rows):
        spread[4 * r : 4 * r + 4, :] = recv_v[r].astype(F32)
    signals = [short(spread[pl.ds(q, rows, stride=4), :], 0, q) for q in range(chan)]

    for order in range(2):
        spectrum = forward(signals)
        re, im = spectrum[:, :BLOCK], spectrum[:, BLOCK:]
        kern_re, kern_im = spectra[order, :, :BLOCK], spectra[order, :, BLOCK:]
        product = jnp.concatenate(
            [re * kern_re - im * kern_im, re * kern_im + im * kern_re], axis=1
        )
        longs = backward(product)
        if order == 0:
            all_of(send_g, recv_g, 1).wait_recv()
            for r in range(rows):
                spread[8 * r : 8 * r + 8, :] = recv_g[r].astype(F32)
        for q in range(chan):
            gate = short(spread[pl.ds(order * chan + q, rows, stride=8), :], 1 + order, q)
            signals[q] = gate * (longs[q] + skip_s[order, row * chan + q] * signals[q])

    for q in range(4):
        spread[pl.ds(q, rows, stride=4), :] = (
            signals[q] if q < chan else jnp.zeros((rows, BLOCK), F32)
        )
    for r in range(rows):
        send_y[r] = spread[4 * r : 4 * r + 4, :].astype(BF16)
    send(send_y, recv_y, 2, 0)
    recv_y[row] = send_y[row]
    all_of(send_y, recv_y, 2).wait_recv()
    for r in range(rows):
        spread[4 * r : 4 * r + 4, :] = recv_y[r].astype(F32)
    for q in range(chan):
        plain[pl.ds(q, rows, stride=chan), :] = spread[pl.ds(q, rows, stride=4), :]
    blocks[col] = plain[...].astype(BF16)

    def to_chip(step):
        return pltpu.make_async_remote_copy(
            src_ref=blocks.at[col],
            dst_ref=blocks.at[col],
            send_sem=near_send.at[step],
            recv_sem=near_recv.at[step],
            device_id=(row, lax.rem(place + step, chips) * 2 + core),
            device_id_type=MESH,
        )

    def to_pair(step):
        own = lax.rem(place + chips - step, chips) * 2 + core
        return pltpu.make_async_remote_copy(
            src_ref=blocks.at[own],
            dst_ref=blocks.at[own],
            send_sem=pair_send.at[step],
            recv_sem=pair_recv.at[step],
            device_id=(row, partner),
            device_id_type=MESH,
        )

    def block_product(index):
        start = pl.multiple_of(index * width, 16)
        return dot(blocks[index], out_v[pl.ds(start, width), :], ((0,), (0,)))

    near_first = [s for d in range(1, chips // 2 + 1) for s in sorted({d, chips - d})]
    for step in near_first[::-1]:
        to_chip(step).start()
    to_pair(0).start()
    loads[4].wait()
    total = block_product(col)
    for step in near_first:
        to_chip(step).wait_recv()
        to_pair(step).start()
        total += block_product(lax.rem(place + chips - step, chips) * 2 + core)
    for step in [0] + near_first:
        to_pair(step).wait_recv()
        total += block_product(lax.rem(place + chips - step, chips) * 2 + 1 - core)
    result[...] = total.astype(BF16)

    for source, landing, which in ((send_v, recv_v, 0), (send_g, recv_g, 1), (send_y, recv_y, 2)):
        all_of(source, landing, which).wait_send()
    for step in near_first:
        to_chip(step).wait_send()
    for step in [0] + near_first:
        to_pair(step).wait_send()


def on_device(
    tokens,
    w_value,
    w_gate_one,
    w_gate_two,
    short_taps,
    filter_in,
    filter_mid,
    filter_out,
    decay_rate,
    skip,
    w_out,
):
    rows, cols = lax.axis_size("row"), lax.axis_size("col")
    row, col = lax.axis_index("row"), lax.axis_index("col")
    width, depth = w_value.shape
    chan = width // rows
    seq_len = rows * BLOCK
    own_out = lax.dynamic_slice_in_dim(filter_out, col * width + row * chan, chan, 3)
    turns = 1 / (2 * math.pi)
    first_w = jnp.concatenate([filter_in[1:], filter_in[:1]]).T * turns
    first_w = jnp.pad(first_w, ((0, 0), (0, 48 - first_w.shape[1])))
    last_w = jnp.pad(own_out.reshape(64, 4 * chan).T, ((0, 16 - 4 * chan), (0, 0)))
    params = jnp.concatenate(
        [
            jnp.pad(jnp.tile(first_w, (1, 3)), ((0, 0), (0, 112))),
            jnp.pad(jnp.tile(filter_mid.T * turns, (1, 3)), ((0, 0), (0, 64))),
            jnp.pad(jnp.tile(last_w, (1, 3)), ((0, 0), (0, 64))),
        ]
    )
    tables = [jnp.asarray(table) for table in constants(rows, seq_len)]
    smem = pl.BlockSpec(memory_space=pltpu.SMEM)
    vmem = pl.BlockSpec(memory_space=pltpu.VMEM)
    hbm = pl.BlockSpec(memory_space=pl.ANY)
    early = min(EARLY, rows // CHUNK_BLOCKS)
    return pl.pallas_call(
        functools.partial(kernel, (rows, cols, chan, early)),
        out_shape=jax.ShapeDtypeStruct((BLOCK, w_out.shape[1]), BF16),
        in_specs=[smem] * 3 + [hbm] * 5 + [vmem] * 7,
        out_specs=vmem,
        scratch_shapes=[
            pltpu.VMEM((BLOCK, depth), BF16),
            pltpu.VMEM((3, width, depth), BF16),
            pltpu.VMEM(w_out.shape, BF16),
            pltpu.VMEM((width, BLOCK), F32),
            pltpu.VMEM((8 * rows, BLOCK), F32),
            pltpu.VMEM((16 * rows, BLOCK), F32),
            pltpu.VMEM((2, width, 2 * BLOCK), F32),
            pltpu.VMEM((rows, 4, BLOCK), BF16),
            pltpu.VMEM((rows, 8, BLOCK), BF16),
            pltpu.VMEM((rows, 4, BLOCK), BF16),
            pltpu.VMEM((rows, 8, BLOCK), BF16),
            pltpu.VMEM((rows, 4, BLOCK), BF16),
            pltpu.VMEM((rows, 4, BLOCK), BF16),
            pltpu.VMEM((cols, width, BLOCK), BF16),
            pltpu.SemaphoreType.DMA((5,)),
            pltpu.SemaphoreType.DMA((3,)),
            pltpu.SemaphoreType.DMA((3,)),
            pltpu.SemaphoreType.DMA((cols // 2,)),
            pltpu.SemaphoreType.DMA((cols // 2,)),
            pltpu.SemaphoreType.DMA((cols // 2,)),
            pltpu.SemaphoreType.DMA((cols // 2,)),
        ],
        compiler_params=pltpu.CompilerParams(collective_id=0, has_side_effects=True),
    )(
        short_taps.reshape(9, width),
        skip,
        decay_rate,
        tokens,
        w_value,
        w_gate_one,
        w_gate_two,
        w_out,
        params,
        *tables,
    )


EARLY = 6


def solution(mesh):
    placed = (
        P("row", None),
        P("col", None),
        P("col", None),
        P("col", None),
        P(None, None, "col"),
        P(),
        P(),
        P(),
        P("col"),
        P(None, "col"),
        P(None, "col"),
    )
    return jax.shard_map(
        on_device, mesh=mesh, in_specs=placed, out_specs=P("row", "col"), check_vma=False
    )
```

```python
import functools
import math

import jax
import jax.numpy as jnp
import ml_dtypes
import numpy as np
from jax import lax
from jax.experimental import pallas as pl
from jax.experimental.pallas import tpu as pltpu
from jax.sharding import PartitionSpec as P

BANDS = 16
BLOCK = 128
CHUNK_BLOCKS = 16
SINE = (
    6.283182818553798,
    -41.341421398897,
    81.59618387742557,
    -76.58010056369793,
    41.20539500742814,
    -12.271262547422271,
)
ROUNDER = 12582912.0
PARCELS = (((0, 0), (0, 1), (0, 2), (1, 0)), ((1, 1), (1, 2), (2, 0), (2, 1)), ((2, 2), None))
MESH = pl.DeviceIdType.MESH
F32 = jnp.float32
BF16 = jnp.bfloat16


def halves(table):
    high = table.astype(ml_dtypes.bfloat16)
    low = (table - high.astype(np.float64)).astype(ml_dtypes.bfloat16)
    return high, low


def constants(rows, seq_len):
    wide = 2 * rows
    total = wide * BLOCK
    odd = np.arange(rows)[:, None] + 0.5
    blocks = np.arange(rows)[None, :]
    one = 2 * np.pi * odd * blocks / wide
    first = np.concatenate([np.cos(one), -np.sin(one)], axis=0)
    last = np.concatenate([np.cos(one).T, -np.sin(one).T], axis=1) * (2.0 / total)
    first_h, first_l = halves(first)
    last_h, last_l = halves(last)
    first = np.concatenate([first_h, first_l, first_h], axis=1)
    last = np.concatenate([last_h, last_l, last_h], axis=1)
    lanes = np.arange(BLOCK)
    two = 2 * np.pi * odd * lanes[None, :] / total
    twiddle = np.stack([np.cos(two), np.sin(two)]).astype(np.float32)
    three = 2 * np.pi * (lanes[:, None] * lanes[None, :] % BLOCK) / BLOCK
    cosine, sine = np.cos(three), np.sin(three)
    forward = np.block([[cosine, -sine], [sine, cosine]])
    inverse = np.block([[cosine, sine], [-sine, cosine]])
    square = np.stack([*halves(forward), *halves(inverse)])
    chunk = CHUNK_BLOCKS * BLOCK
    bands = np.linspace(0.0001, BANDS - 1, BANDS, dtype=np.float32).astype(np.float64)
    rate = 2 * np.pi / seq_len * bands[:, None]
    inside = rate * np.arange(chunk)[None, :]
    base = np.concatenate([np.cos(inside), np.sin(inside)]).astype(np.float32)
    steps = np.arange(seq_len // chunk)[:, None, None] * chunk * rate[None]
    turn = np.concatenate([np.cos(steps), np.sin(steps)], axis=1)
    turn = np.broadcast_to(turn, turn.shape[:2] + (BLOCK,)).astype(np.float32)
    return first, last, twiddle, square, base, np.ascontiguousarray(turn)


def timed(name, wait):
    with jax.named_scope(name):
        wait()


def dot(left, right, dims=((1,), (0,))):
    return lax.dot_general(left, right, (dims, ((), ())), preferred_element_type=F32)


def split(value):
    high = value.astype(BF16)
    return high, (value - high.astype(F32)).astype(BF16)


def sine_of_turns(turns):
    part = turns - ((turns + ROUNDER) - ROUNDER)
    square = part * part
    total = jnp.full_like(square, SINE[-1])
    for coefficient in SINE[-2::-1]:
        total = total * square + coefficient
    return total * part


def stacked(value):
    high, low = split(value)
    return jnp.concatenate([high, high, low], axis=0)


def tripled(weights, width):
    high = weights.astype(BF16).astype(F32)
    lane = lax.broadcasted_iota(jnp.int32, weights.shape, 1)
    middle = (lane >= width) & (lane < 2 * width)
    return jnp.where(middle, weights - high, high).astype(BF16)


def kernel(
    sizes,
    taps_h,
    skip_h,
    rate_h,
    tokens_h,
    value_h,
    gate_one_h,
    gate_two_h,
    out_h,
    filter_in_h,
    filter_mid_h,
    filter_out_h,
    first_h,
    last_h,
    twiddle_h,
    square_h,
    base_h,
    turn_h,
    result,
    taps_s,
    skip_s,
    rate_s,
    filter_in,
    filter_mid,
    filter_out,
    first,
    last,
    twiddle,
    square,
    base,
    turn,
    flip,
    tokens_v,
    weights_v,
    out_v,
    plain,
    spread,
    gathered_taps,
    spectra,
    send_a,
    send_b,
    send_c,
    recv_a,
    recv_b,
    recv_c,
    send_y,
    recv_y,
    blocks,
    load_sem,
    send_sem,
    recv_sem,
    near_send,
    near_recv,
    pair_send,
    pair_recv,
):
    rows, cols, chan = sizes
    width = rows * chan
    chips = cols // 2
    row = lax.axis_index("row")
    col = lax.axis_index("col")
    place = col // 2
    core = col % 2
    partner = place * 2 + 1 - core

    own = col * width + row * chan
    window = jnp.minimum(own // 128, filter_out_h.shape[3] // 128 - 2) * 128
    window = pl.multiple_of(window, 128)
    pairs = [
        (tokens_h, tokens_v),
        (value_h, weights_v.at[0]),
        (gate_one_h, weights_v.at[1]),
        (gate_two_h, weights_v.at[2]),
        (filter_in_h, filter_in),
        (filter_mid_h, filter_mid),
        (filter_out_h.at[:, :, :, pl.ds(window, 256)], filter_out),
        (base_h, base),
        (turn_h, turn),
        (first_h, first),
        (last_h, last),
        (twiddle_h, twiddle),
        (square_h, square),
        (out_h, out_v),
        (rate_h, rate_s),
        (taps_h, taps_s),
        (skip_h, skip_s),
    ]
    loads = [pltpu.make_async_copy(*pair, load_sem.at[at]) for at, pair in enumerate(pairs)]
    for load in loads[:2]:
        load.start()

    barrier = pltpu.get_barrier_semaphore()

    def wrapped(index, extent):
        return jnp.where(index >= extent, index - extent, index)

    def far_first(visit):
        middle = rows // 2
        visit(wrapped(row + middle, rows))

        @pl.loop(1, middle)
        def _(step):
            visit(wrapped(row + middle + step, rows))
            visit(wrapped(row + middle - step, rows))

    def greet(other):
        pl.semaphore_signal(barrier, inc=1, device_id=(other, col), device_id_type=MESH)

    far_first(greet)
    for step in range(1, chips):
        other = wrapped(place + step, chips) * 2 + core
        pl.semaphore_signal(barrier, inc=1, device_id=(row, other), device_id_type=MESH)
    pl.semaphore_signal(barrier, inc=1, device_id=(row, partner), device_id_type=MESH)
    for load in loads[2:]:
        load.start()

    def send(source, landing, which):
        def visit(other):
            pltpu.make_async_remote_copy(
                src_ref=source.at[other],
                dst_ref=landing.at[row],
                send_sem=send_sem.at[which],
                recv_sem=recv_sem.at[which],
                device_id=(other, col),
                device_id_type=MESH,
            ).start()

        far_first(visit)

    def all_of(source, landing, which):
        return pltpu.make_async_remote_copy(
            src_ref=source.at[pl.ds(0, rows - 1)],
            dst_ref=landing.at[pl.ds(0, rows - 1)],
            send_sem=send_sem.at[which],
            recv_sem=recv_sem.at[which],
            device_id=(wrapped(row + 1, rows), col),
            device_id_type=MESH,
        )

    outgoing = (send_a, send_b, send_c)
    incoming = (recv_a, recv_b, recv_c)

    timed("load_tokens", loads[0].wait)
    for which in range(3):
        timed("load_weights", loads[1 + which].wait)
        projected = dot(weights_v[which], tokens_v[...], ((1,), (1,)))
        plain[...] = projected.astype(BF16).astype(F32)
        for parcel, members in enumerate(PARCELS):
            for slot, member in enumerate(members):
                if member is not None and member[0] == which:
                    spread[parcel, pl.ds(slot, rows, stride=len(members)), :] = plain[
                        pl.ds(member[1], rows, stride=chan), :
                    ]
    spread[2, pl.ds(1, rows, stride=2), :] = jnp.zeros((rows, BLOCK), F32)
    for parcel, members in enumerate(PARCELS):
        size = len(members)
        for r in range(rows):
            outgoing[parcel][r] = spread[parcel, size * r : size * r + size, :].astype(BF16)

    n_chunks = rows // CHUNK_BLOCKS
    chunk = CHUNK_BLOCKS * BLOCK
    seq_len = rows * BLOCK
    for load in loads[4:9] + loads[14:15]:
        timed("load_filter", load.wait)
    turns = 1 / (2 * math.pi)
    flip[...] = jnp.zeros_like(flip)
    for copy in range(3):
        flip[48 * copy : 48 * copy + 32, 0:64] = filter_in[1:33, :] * turns
        flip[48 * copy + 32 : 48 * copy + 33, 0:64] = filter_in[0:1, :] * turns
    in_w = tripled(flip[...].T[0:64, 0:144], 48)
    for copy in range(3):
        flip[64 * copy : 64 * copy + 64, 0:64] = filter_mid[...] * turns
    mid_w = tripled(flip[...].T[0:64, 0:192], 64)
    pick_row = lax.broadcasted_iota(jnp.int32, (16, 256), 0)
    pick_lane = lax.broadcasted_iota(jnp.int32, (16, 256), 1)
    out_w = jnp.zeros((16, 192), F32)
    for kind in range(4):
        high, low = split(filter_out[:, kind // 2, kind % 2, :])
        wanted = (pick_row // chan == kind) & (pick_lane == own - window + pick_row % chan)
        pick = jnp.where(wanted, 1.0, 0.0).astype(BF16)
        out_w += dot(pick, jnp.concatenate([high, low, high], axis=0), ((1,), (1,)))
    out_w = out_w.astype(BF16)
    rate_rows = jnp.zeros((16, BLOCK), F32)
    channel = lax.rem(lax.broadcasted_iota(jnp.int32, (16, BLOCK), 0), chan)
    for q in range(chan):
        rate_rows = jnp.where(channel == q, rate_s[row * chan + q], rate_rows)
    rate_rows = jnp.concatenate([rate_rows] * CHUNK_BLOCKS, axis=1)

    def filter_chunk(index):
        lane = lax.broadcasted_iota(jnp.int32, (16, chunk), 1)
        relative = (lane + index * chunk).astype(F32) * (1.0 / (seq_len - 1))
        first_row = lax.broadcasted_iota(jnp.int32, (16, chunk), 0) == 0
        turn_c = jnp.concatenate([turn[index, 0:BANDS, :]] * CHUNK_BLOCKS, axis=1)
        turn_s = jnp.concatenate([turn[index, BANDS : 2 * BANDS, :]] * CHUNK_BLOCKS, axis=1)
        base_c, base_s = base[0:BANDS, :], base[BANDS : 2 * BANDS, :]
        feats = jnp.concatenate(
            [
                base_c * turn_c - base_s * turn_s,
                base_s * turn_c + base_c * turn_s,
                jnp.where(first_row, relative, 0.0),
            ],
            axis=0,
        )
        hidden = sine_of_turns(dot(in_w, stacked(feats)))
        hidden = sine_of_turns(dot(mid_w, stacked(hidden)))
        filter_taps = dot(out_w, stacked(hidden)) * jnp.exp(-relative * rate_rows)
        for b in range(CHUNK_BLOCKS):
            start = pl.multiple_of((index * CHUNK_BLOCKS + b) * 16, 16)
            gathered_taps[pl.ds(start, 16), :] = filter_taps[:, b * BLOCK : (b + 1) * BLOCK]

    timed("barrier", lambda: pl.semaphore_wait(barrier, rows - 1 + chips - 1 + 1))
    for parcel in range(3):
        send(outgoing[parcel], incoming[parcel], parcel)
    for parcel in range(3):
        incoming[parcel][row] = outgoing[parcel][row]

    @pl.loop(0, n_chunks)
    def _(index):
        filter_chunk(index)

    for load in loads[9:13] + loads[15:17]:
        timed("load_tables", load.wait)
    tw_c, tw_s = twiddle[0], twiddle[1]

    def forward(signals):
        reals, imags = [], []
        for signal in signals:
            both = dot(first[...], stacked(signal))
            re, im = both[:rows], both[rows:]
            reals.append(re * tw_c + im * tw_s)
            imags.append(im * tw_c - re * tw_s)
        both = jnp.concatenate(
            [jnp.concatenate(reals, axis=0), jnp.concatenate(imags, axis=0)], axis=1
        )
        high, low = split(both)
        return dot(high, square[0]) + dot(high, square[1]) + dot(low, square[0])

    def backward(spectrum):
        high, low = split(spectrum)
        both = dot(high, square[2]) + dot(high, square[3]) + dot(low, square[2])
        signals = []
        for q in range(chan):
            re = both[q * rows : (q + 1) * rows, :BLOCK]
            im = both[q * rows : (q + 1) * rows, BLOCK:]
            turned = jnp.concatenate([re * tw_c - im * tw_s, im * tw_c + re * tw_s], axis=0)
            signals.append(dot(last[...], stacked(turned)))
        return signals

    lane = lax.broadcasted_iota(jnp.int32, (rows, BLOCK), 1)
    line = lax.broadcasted_iota(jnp.int32, (rows, BLOCK), 0)
    origin = (lane == 0) & (line == 0)
    for order in range(2):
        ahead, behind = [], []
        for q in range(chan):
            base_row = (order * 2) * chan + q
            ahead.append(gathered_taps[pl.ds(base_row, rows, stride=16), :])
            back = gathered_taps[pl.ds(base_row + chan, rows, stride=16), :]
            behind.append(jnp.where(origin, 0.0, back))
        ahead = forward(ahead)
        behind = forward(behind)
        spectra[order, :, :BLOCK] = ahead[:, :BLOCK] + behind[:, :BLOCK]
        spectra[order, :, BLOCK:] = ahead[:, BLOCK:] - behind[:, BLOCK:]

    def short(signal, which, q):
        before = pltpu.roll(signal, 1, 1)
        before = jnp.where(lane == 0, pltpu.roll(before, 1, 0), before)
        before = jnp.where(origin, 0.0, before)
        after = pltpu.roll(signal, BLOCK - 1, 1)
        after = jnp.where(lane == BLOCK - 1, pltpu.roll(after, rows - 1, 0), after)
        after = jnp.where((lane == BLOCK - 1) & (line == rows - 1), 0.0, after)
        at = row * chan + q
        return (
            before * taps_s[which, 0, at]
            + signal * taps_s[which, 1, at]
            + after * taps_s[which, 2, at]
        )

    def unpack(parcel):
        wait = all_of(outgoing[parcel], incoming[parcel], parcel).wait_recv
        timed(f"parcel_{parcel}_in", wait)
        size = len(PARCELS[parcel])
        for r in range(rows):
            spread[parcel, size * r : size * r + size, :] = incoming[parcel][r].astype(F32)

    def shorted(which):
        found = []
        for q in range(chan):
            for parcel, members in enumerate(PARCELS):
                if (which, q) in members:
                    rows_of = pl.ds(members.index((which, q)), rows, stride=len(members))
                    found.append(short(spread[parcel, rows_of, :], which, q))
        return found

    unpack(0)
    signals = shorted(0)
    for order in range(2):
        spectrum = forward(signals)
        re, im = spectrum[:, :BLOCK], spectrum[:, BLOCK:]
        kern_re, kern_im = spectra[order, :, :BLOCK], spectra[order, :, BLOCK:]
        product = jnp.concatenate(
            [re * kern_re - im * kern_im, re * kern_im + im * kern_re], axis=1
        )
        longs = backward(product)
        unpack(1 + order)
        gates = shorted(1 + order)
        for q in range(chan):
            signals[q] = gates[q] * (longs[q] + skip_s[order, row * chan + q] * signals[q])

    for q in range(4):
        spread[0, pl.ds(q, rows, stride=4), :] = (
            signals[q] if q < chan else jnp.zeros((rows, BLOCK), F32)
        )
    for r in range(rows):
        send_y[r] = spread[0, 4 * r : 4 * r + 4, :].astype(BF16)
    send(send_y, recv_y, 3)
    recv_y[row] = send_y[row]
    timed("mixer_in", all_of(send_y, recv_y, 3).wait_recv)
    for r in range(rows):
        spread[0, 4 * r : 4 * r + 4, :] = recv_y[r].astype(F32)
    for q in range(chan):
        plain[pl.ds(q, rows, stride=chan), :] = spread[0, pl.ds(q, rows, stride=4), :]
    blocks[col] = plain[...].astype(BF16)

    def to_chip(step):
        return pltpu.make_async_remote_copy(
            src_ref=blocks.at[col],
            dst_ref=blocks.at[col],
            send_sem=near_send.at[step],
            recv_sem=near_recv.at[step],
            device_id=(row, wrapped(place + step, chips) * 2 + core),
            device_id_type=MESH,
        )

    def source(step):
        return wrapped(place + chips - step, chips)

    def to_pair(step):
        own = source(step) * 2 + core
        return pltpu.make_async_remote_copy(
            src_ref=blocks.at[own],
            dst_ref=blocks.at[own],
            send_sem=pair_send.at[step],
            recv_sem=pair_recv.at[step],
            device_id=(row, partner),
            device_id_type=MESH,
        )

    def product(indices):
        left = jnp.concatenate([blocks[index] for index in indices], axis=0)
        starts = [pl.multiple_of(index * width, 16) for index in indices]
        right = jnp.concatenate([out_v[pl.ds(start, width), :] for start in starts], axis=0)
        return dot(left, right, ((0,), (0,)))

    half = chips // 2
    before = jnp.where(core == 0, half - 1, half + 1)
    after = chips - before
    hand = wrapped(place + chips - before, chips) * 2 + core
    onward = wrapped(place + chips - 1 + 2 * (1 - core), 2 * chips)
    onward = wrapped(onward, chips)

    relay = pltpu.make_async_remote_copy(
        src_ref=blocks.at[hand],
        dst_ref=blocks.at[hand],
        send_sem=near_send.at[half],
        recv_sem=near_recv.at[half],
        device_id=(row, onward * 2 + core),
        device_id_type=MESH,
    )
    steps = [before, after] + [s for d in range(half - 2, 0, -1) for s in (d, chips - d)]
    for step in steps:
        to_chip(step).start()
    to_pair(0).start()
    timed("load_out", loads[13].wait)
    steps.insert(-2, half)
    middle = 3
    total = jnp.zeros((BLOCK, out_v.shape[1]), F32)
    for at, step in enumerate(steps):
        timed("near_in", to_chip(step).wait_recv)
        if at == 0:
            relay.start()
        to_pair(step).start()
        if at == middle:
            total += product([source(s) * 2 + core for s in [0] + steps[: middle + 1]])
    total += product([source(s) * 2 + core for s in steps[middle + 1 :]])
    for group in ([0] + steps[:middle], steps[middle:]):
        for step in group:
            timed("pair_in", to_pair(step).wait_recv)
        total += product([source(step) * 2 + 1 - core for step in group])
    result[...] = total.astype(BF16)

    for parcel in range(3):
        all_of(outgoing[parcel], incoming[parcel], parcel).wait_send()
    timed("drain", all_of(send_y, recv_y, 3).wait_send)
    for step in steps:
        to_chip(step).wait_send()
    for step in [0] + steps:
        to_pair(step).wait_send()


def on_device(
    tokens,
    w_value,
    w_gate_one,
    w_gate_two,
    short_taps,
    filter_in,
    filter_mid,
    filter_out,
    decay_rate,
    skip,
    w_out,
):
    rows, cols = lax.axis_size("row"), lax.axis_size("col")
    width, depth = w_value.shape
    chan = width // rows
    seq_len = rows * BLOCK
    tables = [jnp.asarray(table) for table in constants(rows, seq_len)]
    vmem = pl.BlockSpec(memory_space=pltpu.VMEM)
    hbm = pl.BlockSpec(memory_space=pl.ANY)
    return pl.pallas_call(
        functools.partial(kernel, (rows, cols, chan)),
        out_shape=pltpu.VMEM((BLOCK, w_out.shape[1]), BF16),
        in_specs=[hbm] * 17,
        out_specs=vmem,
        scratch_shapes=[
            pltpu.SMEM(short_taps.shape, F32),
            pltpu.SMEM(skip.shape, F32),
            pltpu.SMEM(decay_rate.shape, F32),
            pltpu.VMEM(filter_in.shape, F32),
            pltpu.VMEM(filter_mid.shape, F32),
            pltpu.VMEM(filter_out.shape[:3] + (256,), F32),
            *[pltpu.VMEM(table.shape, table.dtype) for table in tables],
            pltpu.VMEM((256, 128), F32),
            pltpu.VMEM((BLOCK, depth), BF16),
            pltpu.VMEM((3, width, depth), BF16),
            pltpu.VMEM(w_out.shape, BF16),
            pltpu.VMEM((width, BLOCK), F32),
            pltpu.VMEM((3, 4 * rows, BLOCK), F32),
            pltpu.VMEM((16 * rows, BLOCK), F32),
            pltpu.VMEM((2, width, 2 * BLOCK), F32),
            *[pltpu.VMEM((rows, len(members), BLOCK), BF16) for members in PARCELS],
            *[pltpu.VMEM((rows, len(members), BLOCK), BF16) for members in PARCELS],
            pltpu.VMEM((rows, 4, BLOCK), BF16),
            pltpu.VMEM((rows, 4, BLOCK), BF16),
            pltpu.VMEM((cols, width, BLOCK), BF16),
            pltpu.SemaphoreType.DMA((17,)),
            pltpu.SemaphoreType.DMA((4,)),
            pltpu.SemaphoreType.DMA((4,)),
            pltpu.SemaphoreType.DMA((cols // 2,)),
            pltpu.SemaphoreType.DMA((cols // 2,)),
            pltpu.SemaphoreType.DMA((cols // 2,)),
            pltpu.SemaphoreType.DMA((cols // 2,)),
        ],
        compiler_params=pltpu.CompilerParams(collective_id=0, has_side_effects=True),
    )(
        short_taps,
        skip,
        decay_rate,
        tokens,
        w_value,
        w_gate_one,
        w_gate_two,
        w_out,
        filter_in,
        filter_mid,
        filter_out,
        *tables,
    )


def solution(mesh):
    placed = (
        P("row", None),
        P("col", None),
        P("col", None),
        P("col", None),
        P(None, None, "col"),
        P(),
        P(),
        P(),
        P("col"),
        P(None, "col"),
        P(None, "col"),
    )
    return jax.shard_map(
        on_device, mesh=mesh, in_specs=placed, out_specs=P("row", "col"), check_vma=False
    )
```

```python
import functools
import math

import jax
import jax.numpy as jnp
import ml_dtypes
import numpy as np
from jax import lax
from jax.experimental import pallas as pl
from jax.experimental.pallas import tpu as pltpu
from jax.sharding import PartitionSpec as P

BANDS = 16
BLOCK = 128
CHUNK_BLOCKS = 16
SINE = (
    6.283182818553798,
    -41.341421398897,
    81.59618387742557,
    -76.58010056369793,
    41.20539500742814,
    -12.271262547422271,
)
ROUNDER = 12582912.0
GROUPS = 3
PARCELS = (((0, 0), (0, 1), (0, 2), (1, 0)), ((1, 1), (1, 2), (2, 0), (2, 1)), ((2, 2), None))
MESH = pl.DeviceIdType.MESH
F32 = jnp.float32
BF16 = jnp.bfloat16


def halves(table):
    high = table.astype(ml_dtypes.bfloat16)
    low = (table - high.astype(np.float64)).astype(ml_dtypes.bfloat16)
    return high, low


def constants(rows, seq_len):
    wide = 2 * rows
    total = wide * BLOCK
    odd = np.arange(rows)[:, None] + 0.5
    blocks = np.arange(rows)[None, :]
    one = 2 * np.pi * odd * blocks / wide
    first = np.concatenate([np.cos(one), -np.sin(one)], axis=0)
    last = np.concatenate([np.cos(one).T, -np.sin(one).T], axis=1) * (2.0 / total)
    first_h, first_l = halves(first)
    last_h, last_l = halves(last)
    first = np.concatenate([first_h, first_l, first_h], axis=1)
    last = np.concatenate([last_h, last_l, last_h], axis=1)
    lanes = np.arange(BLOCK)
    two = 2 * np.pi * odd * lanes[None, :] / total
    twiddle = np.stack([np.cos(two), np.sin(two)]).astype(np.float32)
    three = 2 * np.pi * (lanes[:, None] * lanes[None, :] % BLOCK) / BLOCK
    cosine, sine = np.cos(three), np.sin(three)
    forward = np.block([[cosine, -sine], [sine, cosine]])
    inverse = np.block([[cosine, sine], [-sine, cosine]])
    square = np.stack([*halves(forward), *halves(inverse)])
    chunk = CHUNK_BLOCKS * BLOCK
    bands = np.linspace(0.0001, BANDS - 1, BANDS, dtype=np.float32).astype(np.float64)
    rate = 2 * np.pi / seq_len * bands[:, None]
    inside = rate * np.arange(chunk)[None, :]
    base = np.concatenate([np.cos(inside), np.sin(inside)]).astype(np.float32)
    steps = np.arange(seq_len // chunk)[:, None, None] * chunk * rate[None]
    turn = np.concatenate([np.cos(steps), np.sin(steps)], axis=1)
    turn = np.broadcast_to(turn, turn.shape[:2] + (BLOCK,)).astype(np.float32)
    return first, last, twiddle, square, base, np.ascontiguousarray(turn)


def timed(name, wait):
    with jax.named_scope(name):
        wait()


def dot(left, right, dims=((1,), (0,))):
    return lax.dot_general(left, right, (dims, ((), ())), preferred_element_type=F32)


def split(value):
    high = value.astype(BF16)
    return high, (value - high.astype(F32)).astype(BF16)


def sine_of_turns(turns):
    part = turns - ((turns + ROUNDER) - ROUNDER)
    square = part * part
    total = jnp.full_like(square, SINE[-1])
    for coefficient in SINE[-2::-1]:
        total = total * square + coefficient
    return total * part


def stacked(value):
    high, low = split(value)
    return jnp.concatenate([high, high, low], axis=0)


def tripled(weights, width):
    high = weights.astype(BF16).astype(F32)
    lane = lax.broadcasted_iota(jnp.int32, weights.shape, 1)
    middle = (lane >= width) & (lane < 2 * width)
    return jnp.where(middle, weights - high, high).astype(BF16)


def kernel(
    sizes,
    taps_h,
    skip_h,
    rate_h,
    tokens_h,
    value_h,
    gate_one_h,
    gate_two_h,
    out_h,
    filter_in_h,
    filter_mid_h,
    filter_out_h,
    first_h,
    last_h,
    twiddle_h,
    square_h,
    base_h,
    turn_h,
    result,
    taps_s,
    skip_s,
    rate_s,
    filter_in,
    filter_mid,
    filter_out,
    first,
    last,
    twiddle,
    square,
    base,
    turn,
    flip,
    tokens_v,
    weights_v,
    out_v,
    plain,
    spread,
    gathered_taps,
    spectra,
    send_a,
    send_b,
    send_c,
    recv_a,
    recv_b,
    recv_c,
    send_y,
    recv_y,
    blocks,
    load_sem,
    send_sem,
    recv_sem,
    near_send,
    near_recv,
    pair_send,
    pair_recv,
):
    rows, cols, chan = sizes
    width = rows * chan
    chips = cols // 2
    row = lax.axis_index("row")
    col = lax.axis_index("col")
    place = col // 2
    core = col % 2
    partner = place * 2 + 1 - core

    own = col * width + row * chan
    window = jnp.minimum(own // 128, filter_out_h.shape[3] // 128 - 2) * 128
    window = pl.multiple_of(window, 128)
    pairs = [
        (tokens_h, tokens_v),
        (value_h, weights_v.at[0]),
        (gate_one_h, weights_v.at[1]),
        (gate_two_h, weights_v.at[2]),
        (filter_in_h, filter_in),
        (filter_mid_h, filter_mid),
        (filter_out_h.at[:, :, :, pl.ds(window, 256)], filter_out),
        (base_h, base),
        (turn_h, turn),
        (first_h, first),
        (last_h, last),
        (twiddle_h, twiddle),
        (square_h, square),
        (out_h, out_v),
        (rate_h, rate_s),
        (taps_h, taps_s),
        (skip_h, skip_s),
    ]
    loads = [pltpu.make_async_copy(*pair, load_sem.at[at]) for at, pair in enumerate(pairs)]
    for load in loads[:2]:
        load.start()

    barrier = pltpu.get_barrier_semaphore()

    def wrapped(index, extent):
        return jnp.where(index >= extent, index - extent, index)

    def far_first(visit):
        middle = rows // 2
        visit(wrapped(row + middle, rows))

        @pl.loop(1, middle)
        def _(step):
            visit(wrapped(row + middle + step, rows))
            visit(wrapped(row + middle - step, rows))

    def greet(other):
        pl.semaphore_signal(barrier, inc=1, device_id=(other, col), device_id_type=MESH)

    far_first(greet)
    for step in range(1, chips):
        other = wrapped(place + step, chips) * 2 + core
        pl.semaphore_signal(barrier, inc=1, device_id=(row, other), device_id_type=MESH)
    pl.semaphore_signal(barrier, inc=1, device_id=(row, partner), device_id_type=MESH)
    for load in loads[2:]:
        load.start()

    def send(source, landing, which, landed):
        def visit(other):
            pltpu.make_async_remote_copy(
                src_ref=source.at[other],
                dst_ref=landing.at[row],
                send_sem=send_sem.at[which],
                recv_sem=recv_sem.at[landed],
                device_id=(other, col),
                device_id_type=MESH,
            ).start()

        far_first(visit)

    def all_of(source, landing, which):
        return pltpu.make_async_remote_copy(
            src_ref=source.at[pl.ds(0, rows - 1)],
            dst_ref=landing.at[pl.ds(0, rows - 1)],
            send_sem=send_sem.at[which],
            recv_sem=recv_sem.at[which],
            device_id=(wrapped(row + 1, rows), col),
            device_id_type=MESH,
        )

    outgoing = (send_a, send_b, send_c)
    incoming = (recv_a, recv_b, recv_c)

    timed("load_tokens", loads[0].wait)
    for which in range(3):
        timed("load_weights", loads[1 + which].wait)
        projected = dot(weights_v[which], tokens_v[...], ((1,), (1,)))
        plain[...] = projected.astype(BF16).astype(F32)
        for parcel, members in enumerate(PARCELS):
            for slot, member in enumerate(members):
                if member is not None and member[0] == which:
                    spread[parcel, pl.ds(slot, rows, stride=len(members)), :] = plain[
                        pl.ds(member[1], rows, stride=chan), :
                    ]
    spread[2, pl.ds(1, rows, stride=2), :] = jnp.zeros((rows, BLOCK), F32)
    for parcel, members in enumerate(PARCELS):
        size = len(members)
        for r in range(rows):
            outgoing[parcel][r] = spread[parcel, size * r : size * r + size, :].astype(BF16)

    n_chunks = rows // CHUNK_BLOCKS
    chunk = CHUNK_BLOCKS * BLOCK
    seq_len = rows * BLOCK
    for load in loads[4:9] + loads[14:15]:
        timed("load_filter", load.wait)
    turns = 1 / (2 * math.pi)
    flip[...] = jnp.zeros_like(flip)
    for copy in range(3):
        flip[48 * copy : 48 * copy + 32, 0:64] = filter_in[1:33, :] * turns
        flip[48 * copy + 32 : 48 * copy + 33, 0:64] = filter_in[0:1, :] * turns
    in_w = tripled(flip[...].T[0:64, 0:144], 48)
    for copy in range(3):
        flip[64 * copy : 64 * copy + 64, 0:64] = filter_mid[...] * turns
    mid_w = tripled(flip[...].T[0:64, 0:192], 64)
    pick_row = lax.broadcasted_iota(jnp.int32, (16, 256), 0)
    pick_lane = lax.broadcasted_iota(jnp.int32, (16, 256), 1)
    out_w = jnp.zeros((16, 192), F32)
    for kind in range(4):
        high, low = split(filter_out[:, kind // 2, kind % 2, :])
        wanted = (pick_row // chan == kind) & (pick_lane == own - window + pick_row % chan)
        pick = jnp.where(wanted, 1.0, 0.0).astype(BF16)
        out_w += dot(pick, jnp.concatenate([high, low, high], axis=0), ((1,), (1,)))
    out_w = out_w.astype(BF16)
    rate_rows = jnp.zeros((16, BLOCK), F32)
    channel = lax.rem(lax.broadcasted_iota(jnp.int32, (16, BLOCK), 0), chan)
    for q in range(chan):
        rate_rows = jnp.where(channel == q, rate_s[row * chan + q], rate_rows)
    rate_rows = jnp.concatenate([rate_rows] * CHUNK_BLOCKS, axis=1)

    def filter_chunk(index):
        lane = lax.broadcasted_iota(jnp.int32, (16, chunk), 1)
        relative = (lane + index * chunk).astype(F32) * (1.0 / (seq_len - 1))
        first_row = lax.broadcasted_iota(jnp.int32, (16, chunk), 0) == 0
        turn_c = jnp.concatenate([turn[index, 0:BANDS, :]] * CHUNK_BLOCKS, axis=1)
        turn_s = jnp.concatenate([turn[index, BANDS : 2 * BANDS, :]] * CHUNK_BLOCKS, axis=1)
        base_c, base_s = base[0:BANDS, :], base[BANDS : 2 * BANDS, :]
        feats = jnp.concatenate(
            [
                base_c * turn_c - base_s * turn_s,
                base_s * turn_c + base_c * turn_s,
                jnp.where(first_row, relative, 0.0),
            ],
            axis=0,
        )
        hidden = sine_of_turns(dot(in_w, stacked(feats)))
        hidden = sine_of_turns(dot(mid_w, stacked(hidden)))
        filter_taps = dot(out_w, stacked(hidden)) * jnp.exp(-relative * rate_rows)
        for b in range(CHUNK_BLOCKS):
            start = pl.multiple_of((index * CHUNK_BLOCKS + b) * 16, 16)
            gathered_taps[pl.ds(start, 16), :] = filter_taps[:, b * BLOCK : (b + 1) * BLOCK]

    timed("barrier", lambda: pl.semaphore_wait(barrier, rows - 1 + chips - 1 + 1))
    for parcel in range(3):
        send(outgoing[parcel], incoming[parcel], parcel, parcel)
    for parcel in range(3):
        incoming[parcel][row] = outgoing[parcel][row]

    @pl.loop(0, n_chunks)
    def _(index):
        filter_chunk(index)

    for load in loads[9:13] + loads[15:17]:
        timed("load_tables", load.wait)
    tw_c, tw_s = twiddle[0], twiddle[1]

    def forward(signals):
        reals, imags = [], []
        for signal in signals:
            both = dot(first[...], stacked(signal))
            re, im = both[:rows], both[rows:]
            reals.append(re * tw_c + im * tw_s)
            imags.append(im * tw_c - re * tw_s)
        both = jnp.concatenate(
            [jnp.concatenate(reals, axis=0), jnp.concatenate(imags, axis=0)], axis=1
        )
        high, low = split(both)
        return dot(high, square[0]) + dot(high, square[1]) + dot(low, square[0])

    def backward(spectrum):
        high, low = split(spectrum)
        both = dot(high, square[2]) + dot(high, square[3]) + dot(low, square[2])
        signals = []
        for q in range(chan):
            re = both[q * rows : (q + 1) * rows, :BLOCK]
            im = both[q * rows : (q + 1) * rows, BLOCK:]
            turned = jnp.concatenate([re * tw_c - im * tw_s, im * tw_c + re * tw_s], axis=0)
            signals.append(dot(last[...], stacked(turned)))
        return signals

    lane = lax.broadcasted_iota(jnp.int32, (rows, BLOCK), 1)
    line = lax.broadcasted_iota(jnp.int32, (rows, BLOCK), 0)
    origin = (lane == 0) & (line == 0)
    for order in range(2):
        ahead, behind = [], []
        for q in range(chan):
            base_row = (order * 2) * chan + q
            ahead.append(gathered_taps[pl.ds(base_row, rows, stride=16), :])
            back = gathered_taps[pl.ds(base_row + chan, rows, stride=16), :]
            behind.append(jnp.where(origin, 0.0, back))
        ahead = forward(ahead)
        behind = forward(behind)
        spectra[order, :, :BLOCK] = ahead[:, :BLOCK] + behind[:, :BLOCK]
        spectra[order, :, BLOCK:] = ahead[:, BLOCK:] - behind[:, BLOCK:]

    def short(signal, which, q):
        before = pltpu.roll(signal, 1, 1)
        before = jnp.where(lane == 0, pltpu.roll(before, 1, 0), before)
        before = jnp.where(origin, 0.0, before)
        after = pltpu.roll(signal, BLOCK - 1, 1)
        after = jnp.where(lane == BLOCK - 1, pltpu.roll(after, rows - 1, 0), after)
        after = jnp.where((lane == BLOCK - 1) & (line == rows - 1), 0.0, after)
        at = row * chan + q
        return (
            before * taps_s[which, 0, at]
            + signal * taps_s[which, 1, at]
            + after * taps_s[which, 2, at]
        )

    def unpack(parcel):
        wait = all_of(outgoing[parcel], incoming[parcel], parcel).wait_recv
        timed(f"parcel_{parcel}_in", wait)
        size = len(PARCELS[parcel])
        for r in range(rows):
            spread[parcel, size * r : size * r + size, :] = incoming[parcel][r].astype(F32)

    def shorted(which):
        found = []
        for q in range(chan):
            for parcel, members in enumerate(PARCELS):
                if (which, q) in members:
                    rows_of = pl.ds(members.index((which, q)), rows, stride=len(members))
                    found.append(short(spread[parcel, rows_of, :], which, q))
        return found

    unpack(0)
    signals = shorted(0)
    for order in range(2):
        spectrum = forward(signals)
        re, im = spectrum[:, :BLOCK], spectrum[:, BLOCK:]
        kern_re, kern_im = spectra[order, :, :BLOCK], spectra[order, :, BLOCK:]
        product = jnp.concatenate(
            [re * kern_re - im * kern_im, re * kern_im + im * kern_re], axis=1
        )
        longs = backward(product)
        unpack(1 + order)
        gates = shorted(1 + order)
        for q in range(chan):
            signals[q] = gates[q] * (longs[q] + skip_s[order, row * chan + q] * signals[q])

    for q in range(4):
        spread[0, pl.ds(q, rows, stride=4), :] = (
            signals[q] if q < chan else jnp.zeros((rows, BLOCK), F32)
        )
    for r in range(rows):
        send_y[r] = spread[0, 4 * r : 4 * r + 4, :].astype(BF16)
    near = rows // GROUPS
    share = near * chan
    mine = lax.div(row, near)
    send(send_y, recv_y, 3, 3 + mine)
    recv_y[row] = send_y[row]

    def source(step):
        return wrapped(place + chips - step, chips)

    lower = wrapped(mine + GROUPS - 1, GROUPS)
    upper = wrapped(mine + 1, GROUPS)
    low_half = row - mine * near < near // 2
    groups = [mine, jnp.where(low_half, lower, upper), jnp.where(low_half, upper, lower)]

    def to_chip(at, step):
        return pltpu.make_async_remote_copy(
            src_ref=blocks.at[col, groups[at]],
            dst_ref=blocks.at[col, groups[at]],
            send_sem=near_send,
            recv_sem=near_recv.at[at, step],
            device_id=(row, wrapped(place + step, chips) * 2 + core),
            device_id_type=MESH,
        )

    def to_pair(at, step):
        own = source(step) * 2 + core
        return pltpu.make_async_remote_copy(
            src_ref=blocks.at[own, groups[at]],
            dst_ref=blocks.at[own, groups[at]],
            send_sem=pair_send,
            recv_sem=pair_recv.at[at, step],
            device_id=(row, partner),
            device_id_type=MESH,
        )

    def product(at, indices):
        left = jnp.concatenate([blocks[index, groups[at]] for index in indices], axis=0)
        starts = [pl.multiple_of(index * width + groups[at] * share, 16) for index in indices]
        right = jnp.concatenate([out_v[pl.ds(start, share), :] for start in starts], axis=0)
        return dot(left, right, ((0,), (0,)))

    steps = [chips // 2] + [s for d in range(chips // 2 - 1, 0, -1) for s in (d, chips - d)]
    for at in range(GROUPS):
        arrivals = recv_y.at[pl.ds(0, near - 1 if at == 0 else near)]
        group_in = pltpu.make_async_remote_copy(
            src_ref=arrivals,
            dst_ref=arrivals,
            send_sem=send_sem.at[3],
            recv_sem=recv_sem.at[3 + groups[at]],
            device_id=(wrapped(row + 1, rows), col),
            device_id_type=MESH,
        )
        timed(f"group_{at}_in", group_in.wait_recv)
        for r in range(near):
            spread[at, 4 * r : 4 * r + 4, :] = recv_y[groups[at] * near + r].astype(F32)
        for q in range(chan):
            plain[pl.ds(at * share + q, near, stride=chan), :] = spread[
                at, pl.ds(q, near, stride=4), :
            ]
        blocks[col, groups[at]] = plain[at * share : (at + 1) * share, :].astype(BF16)
        for step in steps:
            to_chip(at, step).start()
        to_pair(at, 0).start()
    timed("load_out", loads[13].wait)
    for parcel in range(3):
        all_of(outgoing[parcel], incoming[parcel], parcel).wait_send()
    timed("drain", all_of(send_y, recv_y, 3).wait_send)
    total = jnp.zeros((BLOCK, out_v.shape[1]), F32)
    for at in range(GROUPS):
        for step in steps:
            timed("near_in", to_chip(at, step).wait_recv)
            to_pair(at, step).start()
        if at > 0:
            for step in [0] + steps:
                timed("pair_in", to_pair(at - 1, step).wait_recv)
            total += product(at - 1, [source(step) * 2 + 1 - core for step in [0] + steps])
        total += product(at, [source(step) * 2 + core for step in [0] + steps])
    for step in [0] + steps:
        timed("pair_in", to_pair(GROUPS - 1, step).wait_recv)
    total += product(GROUPS - 1, [source(step) * 2 + 1 - core for step in [0] + steps])
    result[...] = total.astype(BF16)

    for sent, sem in ((steps, near_send), ([0] + steps, pair_send)):
        sent = blocks.at[pl.ds(0, len(sent))]
        pltpu.make_async_remote_copy(
            src_ref=sent,
            dst_ref=sent,
            send_sem=sem,
            recv_sem=recv_sem.at[0],
            device_id=(row, partner),
            device_id_type=MESH,
        ).wait_send()


def on_device(
    tokens,
    w_value,
    w_gate_one,
    w_gate_two,
    short_taps,
    filter_in,
    filter_mid,
    filter_out,
    decay_rate,
    skip,
    w_out,
):
    rows, cols = lax.axis_size("row"), lax.axis_size("col")
    width, depth = w_value.shape
    chan = width // rows
    seq_len = rows * BLOCK
    tables = [jnp.asarray(table) for table in constants(rows, seq_len)]
    vmem = pl.BlockSpec(memory_space=pltpu.VMEM)
    hbm = pl.BlockSpec(memory_space=pl.ANY)
    return pl.pallas_call(
        functools.partial(kernel, (rows, cols, chan)),
        out_shape=pltpu.VMEM((BLOCK, w_out.shape[1]), BF16),
        in_specs=[hbm] * 17,
        out_specs=vmem,
        scratch_shapes=[
            pltpu.SMEM(short_taps.shape, F32),
            pltpu.SMEM(skip.shape, F32),
            pltpu.SMEM(decay_rate.shape, F32),
            pltpu.VMEM(filter_in.shape, F32),
            pltpu.VMEM(filter_mid.shape, F32),
            pltpu.VMEM(filter_out.shape[:3] + (256,), F32),
            *[pltpu.VMEM(table.shape, table.dtype) for table in tables],
            pltpu.VMEM((256, 128), F32),
            pltpu.VMEM((BLOCK, depth), BF16),
            pltpu.VMEM((3, width, depth), BF16),
            pltpu.VMEM(w_out.shape, BF16),
            pltpu.VMEM((width, BLOCK), F32),
            pltpu.VMEM((3, 4 * rows, BLOCK), F32),
            pltpu.VMEM((16 * rows, BLOCK), F32),
            pltpu.VMEM((2, width, 2 * BLOCK), F32),
            *[pltpu.VMEM((rows, len(members), BLOCK), BF16) for members in PARCELS],
            *[pltpu.VMEM((rows, len(members), BLOCK), BF16) for members in PARCELS],
            pltpu.VMEM((rows, 4, BLOCK), BF16),
            pltpu.VMEM((rows, 4, BLOCK), BF16),
            pltpu.VMEM((cols, GROUPS, width // GROUPS, BLOCK), BF16),
            pltpu.SemaphoreType.DMA((17,)),
            pltpu.SemaphoreType.DMA((4,)),
            pltpu.SemaphoreType.DMA((3 + GROUPS,)),
            pltpu.SemaphoreType.DMA,
            pltpu.SemaphoreType.DMA((GROUPS, cols // 2)),
            pltpu.SemaphoreType.DMA,
            pltpu.SemaphoreType.DMA((GROUPS, cols // 2)),
        ],
        compiler_params=pltpu.CompilerParams(collective_id=0, has_side_effects=True),
    )(
        short_taps,
        skip,
        decay_rate,
        tokens,
        w_value,
        w_gate_one,
        w_gate_two,
        w_out,
        filter_in,
        filter_mid,
        filter_out,
        *tables,
    )


def solution(mesh):
    placed = (
        P("row", None),
        P("col", None),
        P("col", None),
        P("col", None),
        P(None, None, "col"),
        P(),
        P(),
        P(),
        P("col"),
        P(None, "col"),
        P(None, "col"),
    )
    return jax.shard_map(
        on_device, mesh=mesh, in_specs=placed, out_specs=P("row", "col"), check_vma=False
    )
```

```python
import functools
import math

import jax
import jax.numpy as jnp
import ml_dtypes
import numpy as np
from jax import lax
from jax.experimental import pallas as pl
from jax.experimental.pallas import tpu as pltpu
from jax.sharding import PartitionSpec as P

BANDS = 16
BLOCK = 128
CHUNK_BLOCKS = 16
SINE = (
    6.283182818553798,
    -41.341421398897,
    81.59618387742557,
    -76.58010056369793,
    41.20539500742814,
    -12.271262547422271,
)
ROUNDER = 12582912.0
GROUPS = 3
PARCELS = (((0, 0), (0, 1), (0, 2), (1, 0)), ((1, 1), (1, 2), (2, 0), (2, 1)), ((2, 2), None))
MESH = pl.DeviceIdType.MESH
F32 = jnp.float32
BF16 = jnp.bfloat16


def halves(table):
    high = table.astype(ml_dtypes.bfloat16)
    low = (table - high.astype(np.float64)).astype(ml_dtypes.bfloat16)
    return high, low


def constants(rows, seq_len):
    wide = 2 * rows
    total = wide * BLOCK
    odd = np.arange(rows)[:, None] + 0.5
    blocks = np.arange(rows)[None, :]
    one = 2 * np.pi * odd * blocks / wide
    first = np.concatenate([np.cos(one), -np.sin(one)], axis=0)
    last = np.concatenate([np.cos(one).T, -np.sin(one).T], axis=1) * (2.0 / total)
    first_h, first_l = halves(first)
    last_h, last_l = halves(last)
    first = np.concatenate([first_h, first_l, first_h], axis=1)
    last = np.concatenate([last_h, last_l, last_h], axis=1)
    lanes = np.arange(BLOCK)
    two = 2 * np.pi * odd * lanes[None, :] / total
    twiddle = np.stack([np.cos(two), np.sin(two)]).astype(np.float32)
    three = 2 * np.pi * (lanes[:, None] * lanes[None, :] % BLOCK) / BLOCK
    cosine, sine = np.cos(three), np.sin(three)
    forward = np.block([[cosine, -sine], [sine, cosine]])
    inverse = np.block([[cosine, sine], [-sine, cosine]])
    square = np.stack([*halves(forward), *halves(inverse)])
    chunk = CHUNK_BLOCKS * BLOCK
    bands = np.linspace(0.0001, BANDS - 1, BANDS, dtype=np.float32).astype(np.float64)
    rate = 2 * np.pi / seq_len * bands[:, None]
    inside = rate * np.arange(chunk)[None, :]
    base = np.concatenate([np.cos(inside), np.sin(inside)]).astype(np.float32)
    steps = np.arange(seq_len // chunk)[:, None, None] * chunk * rate[None]
    turn = np.concatenate([np.cos(steps), np.sin(steps)], axis=1)
    turn = np.broadcast_to(turn, turn.shape[:2] + (BLOCK,)).astype(np.float32)
    return first, last, twiddle, square, base, np.ascontiguousarray(turn)


def timed(name, wait):
    with jax.named_scope(name):
        wait()


def dot(left, right, dims=((1,), (0,))):
    return lax.dot_general(left, right, (dims, ((), ())), preferred_element_type=F32)


def split(value):
    high = value.astype(BF16)
    return high, (value - high.astype(F32)).astype(BF16)


def sine_of_turns(turns):
    part = turns - ((turns + ROUNDER) - ROUNDER)
    square = part * part
    total = jnp.full_like(square, SINE[-1])
    for coefficient in SINE[-2::-1]:
        total = total * square + coefficient
    return total * part


def stacked(value):
    high, low = split(value)
    return jnp.concatenate([high, high, low], axis=0)


def tripled(weights, width):
    high = weights.astype(BF16).astype(F32)
    lane = lax.broadcasted_iota(jnp.int32, weights.shape, 1)
    middle = (lane >= width) & (lane < 2 * width)
    return jnp.where(middle, weights - high, high).astype(BF16)


def kernel(
    sizes,
    taps_h,
    skip_h,
    rate_h,
    tokens_h,
    value_h,
    gate_one_h,
    gate_two_h,
    out_h,
    filter_in_h,
    filter_mid_h,
    filter_out_h,
    first_h,
    last_h,
    twiddle_h,
    square_h,
    base_h,
    turn_h,
    result,
    taps_s,
    skip_s,
    rate_s,
    filter_in,
    filter_mid,
    filter_out,
    first,
    last,
    twiddle,
    square,
    base,
    turn,
    flip,
    tokens_v,
    weights_v,
    out_v,
    plain,
    spread,
    gathered_taps,
    spectra,
    send_a,
    send_b,
    send_c,
    recv_a,
    recv_b,
    recv_c,
    send_y,
    recv_y,
    blocks,
    load_sem,
    send_sem,
    recv_sem,
    near_send,
    near_recv,
    pair_send,
    pair_recv,
):
    rows, cols, chan = sizes
    width = rows * chan
    chips = cols // 2
    row = lax.axis_index("row")
    col = lax.axis_index("col")
    place = col // 2
    core = col % 2
    partner = place * 2 + 1 - core

    own = col * width + row * chan
    window = jnp.minimum(own // 128, filter_out_h.shape[3] // 128 - 2) * 128
    window = pl.multiple_of(window, 128)
    pairs = [
        (tokens_h, tokens_v),
        (value_h, weights_v.at[0]),
        (gate_one_h, weights_v.at[1]),
        (gate_two_h, weights_v.at[2]),
        (filter_in_h, filter_in),
        (filter_mid_h, filter_mid),
        (filter_out_h.at[:, :, :, pl.ds(window, 256)], filter_out),
        (base_h, base),
        (turn_h, turn),
        (first_h, first),
        (last_h, last),
        (twiddle_h, twiddle),
        (square_h, square),
        (out_h, out_v),
        (rate_h, rate_s),
        (taps_h, taps_s),
        (skip_h, skip_s),
    ]
    loads = [pltpu.make_async_copy(*pair, load_sem.at[at]) for at, pair in enumerate(pairs)]
    for load in loads[:2]:
        load.start()

    barrier = pltpu.get_barrier_semaphore()

    def wrapped(index, extent):
        return jnp.where(index >= extent, index - extent, index)

    def far_first(visit):
        middle = rows // 2
        visit(wrapped(row + middle, rows))

        @pl.loop(1, middle)
        def _(step):
            visit(wrapped(row + middle + step, rows))
            visit(wrapped(row + middle - step, rows))

    def greet(other):
        pl.semaphore_signal(barrier, inc=1, device_id=(other, col), device_id_type=MESH)

    far_first(greet)
    for step in range(1, chips):
        other = wrapped(place + step, chips) * 2 + core
        pl.semaphore_signal(barrier, inc=1, device_id=(row, other), device_id_type=MESH)
    pl.semaphore_signal(barrier, inc=1, device_id=(row, partner), device_id_type=MESH)
    for load in loads[2:]:
        load.start()

    def send(source, landing, which, landed):
        def visit(other):
            pltpu.make_async_remote_copy(
                src_ref=source.at[other],
                dst_ref=landing.at[row],
                send_sem=send_sem.at[which],
                recv_sem=recv_sem.at[landed],
                device_id=(other, col),
                device_id_type=MESH,
            ).start()

        far_first(visit)

    def all_of(source, landing, which):
        return pltpu.make_async_remote_copy(
            src_ref=source.at[pl.ds(0, rows - 1)],
            dst_ref=landing.at[pl.ds(0, rows - 1)],
            send_sem=send_sem.at[which],
            recv_sem=recv_sem.at[which],
            device_id=(wrapped(row + 1, rows), col),
            device_id_type=MESH,
        )

    outgoing = (send_a, send_b, send_c)
    incoming = (recv_a, recv_b, recv_c)

    timed("load_tokens", loads[0].wait)
    for which in range(3):
        timed("load_weights", loads[1 + which].wait)
        projected = dot(weights_v[which], tokens_v[...], ((1,), (1,)))
        plain[...] = projected.astype(BF16).astype(F32)
        for parcel, members in enumerate(PARCELS):
            for slot, member in enumerate(members):
                if member is not None and member[0] == which:
                    spread[parcel, pl.ds(slot, rows, stride=len(members)), :] = plain[
                        pl.ds(member[1], rows, stride=chan), :
                    ]
    spread[2, pl.ds(1, rows, stride=2), :] = jnp.zeros((rows, BLOCK), F32)
    for parcel, members in enumerate(PARCELS):
        size = len(members)
        for r in range(rows):
            outgoing[parcel][r] = spread[parcel, size * r : size * r + size, :].astype(BF16)

    n_chunks = rows // CHUNK_BLOCKS
    chunk = CHUNK_BLOCKS * BLOCK
    seq_len = rows * BLOCK
    for load in loads[4:9] + loads[14:15]:
        timed("load_filter", load.wait)
    turns = 1 / (2 * math.pi)
    flip[...] = jnp.zeros_like(flip)
    for copy in range(3):
        flip[48 * copy : 48 * copy + 32, 0:64] = filter_in[1:33, :] * turns
        flip[48 * copy + 32 : 48 * copy + 33, 0:64] = filter_in[0:1, :] * turns
    in_w = tripled(flip[...].T[0:64, 0:144], 48)
    for copy in range(3):
        flip[64 * copy : 64 * copy + 64, 0:64] = filter_mid[...] * turns
    mid_w = tripled(flip[...].T[0:64, 0:192], 64)
    pick_row = lax.broadcasted_iota(jnp.int32, (16, 256), 0)
    pick_lane = lax.broadcasted_iota(jnp.int32, (16, 256), 1)
    out_w = jnp.zeros((16, 192), F32)
    for kind in range(4):
        high, low = split(filter_out[:, kind // 2, kind % 2, :])
        wanted = (pick_row // chan == kind) & (pick_lane == own - window + pick_row % chan)
        pick = jnp.where(wanted, 1.0, 0.0).astype(BF16)
        out_w += dot(pick, jnp.concatenate([high, low, high], axis=0), ((1,), (1,)))
    out_w = out_w.astype(BF16)
    rate_rows = jnp.zeros((16, BLOCK), F32)
    channel = lax.rem(lax.broadcasted_iota(jnp.int32, (16, BLOCK), 0), chan)
    for q in range(chan):
        rate_rows = jnp.where(channel == q, rate_s[row * chan + q], rate_rows)
    rate_rows = jnp.concatenate([rate_rows] * CHUNK_BLOCKS, axis=1)

    def filter_chunk(index):
        lane = lax.broadcasted_iota(jnp.int32, (16, chunk), 1)
        relative = (lane + index * chunk).astype(F32) * (1.0 / (seq_len - 1))
        first_row = lax.broadcasted_iota(jnp.int32, (16, chunk), 0) == 0
        turn_c = jnp.concatenate([turn[index, 0:BANDS, :]] * CHUNK_BLOCKS, axis=1)
        turn_s = jnp.concatenate([turn[index, BANDS : 2 * BANDS, :]] * CHUNK_BLOCKS, axis=1)
        base_c, base_s = base[0:BANDS, :], base[BANDS : 2 * BANDS, :]
        feats = jnp.concatenate(
            [
                base_c * turn_c - base_s * turn_s,
                base_s * turn_c + base_c * turn_s,
                jnp.where(first_row, relative, 0.0),
            ],
            axis=0,
        )
        hidden = sine_of_turns(dot(in_w, stacked(feats)))
        hidden = sine_of_turns(dot(mid_w, stacked(hidden)))
        filter_taps = dot(out_w, stacked(hidden)) * jnp.exp(-relative * rate_rows)
        for b in range(CHUNK_BLOCKS):
            start = pl.multiple_of((index * CHUNK_BLOCKS + b) * 16, 16)
            gathered_taps[pl.ds(start, 16), :] = filter_taps[:, b * BLOCK : (b + 1) * BLOCK]

    timed("barrier", lambda: pl.semaphore_wait(barrier, rows - 1 + chips - 1 + 1))
    for parcel in range(3):
        send(outgoing[parcel], incoming[parcel], parcel, parcel)
    for parcel in range(3):
        incoming[parcel][row] = outgoing[parcel][row]

    @pl.loop(0, n_chunks)
    def _(index):
        filter_chunk(index)

    for load in loads[9:13] + loads[15:17]:
        timed("load_tables", load.wait)
    tw_c, tw_s = twiddle[0], twiddle[1]

    def forward(signals):
        reals, imags = [], []
        for signal in signals:
            both = dot(first[...], stacked(signal))
            re, im = both[:rows], both[rows:]
            reals.append(re * tw_c + im * tw_s)
            imags.append(im * tw_c - re * tw_s)
        both = jnp.concatenate(
            [jnp.concatenate(reals, axis=0), jnp.concatenate(imags, axis=0)], axis=1
        )
        high, low = split(both)
        return dot(high, square[0]) + dot(high, square[1]) + dot(low, square[0])

    def backward(spectrum):
        high, low = split(spectrum)
        both = dot(high, square[2]) + dot(high, square[3]) + dot(low, square[2])
        signals = []
        for q in range(chan):
            re = both[q * rows : (q + 1) * rows, :BLOCK]
            im = both[q * rows : (q + 1) * rows, BLOCK:]
            turned = jnp.concatenate([re * tw_c - im * tw_s, im * tw_c + re * tw_s], axis=0)
            signals.append(dot(last[...], stacked(turned)))
        return signals

    lane = lax.broadcasted_iota(jnp.int32, (rows, BLOCK), 1)
    line = lax.broadcasted_iota(jnp.int32, (rows, BLOCK), 0)
    origin = (lane == 0) & (line == 0)
    for order in range(2):
        ahead, behind = [], []
        for q in range(chan):
            base_row = (order * 2) * chan + q
            ahead.append(gathered_taps[pl.ds(base_row, rows, stride=16), :])
            back = gathered_taps[pl.ds(base_row + chan, rows, stride=16), :]
            behind.append(jnp.where(origin, 0.0, back))
        ahead = forward(ahead)
        behind = forward(behind)
        spectra[order, :, :BLOCK] = ahead[:, :BLOCK] + behind[:, :BLOCK]
        spectra[order, :, BLOCK:] = ahead[:, BLOCK:] - behind[:, BLOCK:]

    def short(signal, which, q):
        before = pltpu.roll(signal, 1, 1)
        before = jnp.where(lane == 0, pltpu.roll(before, 1, 0), before)
        before = jnp.where(origin, 0.0, before)
        after = pltpu.roll(signal, BLOCK - 1, 1)
        after = jnp.where(lane == BLOCK - 1, pltpu.roll(after, rows - 1, 0), after)
        after = jnp.where((lane == BLOCK - 1) & (line == rows - 1), 0.0, after)
        at = row * chan + q
        return (
            before * taps_s[which, 0, at]
            + signal * taps_s[which, 1, at]
            + after * taps_s[which, 2, at]
        )

    def unpack(parcel):
        wait = all_of(outgoing[parcel], incoming[parcel], parcel).wait_recv
        timed(f"parcel_{parcel}_in", wait)
        size = len(PARCELS[parcel])
        for r in range(rows):
            spread[parcel, size * r : size * r + size, :] = incoming[parcel][r].astype(F32)

    def shorted(which):
        found = []
        for q in range(chan):
            for parcel, members in enumerate(PARCELS):
                if (which, q) in members:
                    rows_of = pl.ds(members.index((which, q)), rows, stride=len(members))
                    found.append(short(spread[parcel, rows_of, :], which, q))
        return found

    unpack(0)
    signals = shorted(0)
    for order in range(2):
        spectrum = forward(signals)
        re, im = spectrum[:, :BLOCK], spectrum[:, BLOCK:]
        kern_re, kern_im = spectra[order, :, :BLOCK], spectra[order, :, BLOCK:]
        product = jnp.concatenate(
            [re * kern_re - im * kern_im, re * kern_im + im * kern_re], axis=1
        )
        longs = backward(product)
        unpack(1 + order)
        gates = shorted(1 + order)
        for q in range(chan):
            signals[q] = gates[q] * (longs[q] + skip_s[order, row * chan + q] * signals[q])

    for q in range(4):
        spread[0, pl.ds(q, rows, stride=4), :] = (
            signals[q] if q < chan else jnp.zeros((rows, BLOCK), F32)
        )
    for r in range(rows):
        send_y[r] = spread[0, 4 * r : 4 * r + 4, :].astype(BF16)
    near = rows // GROUPS
    share = near * chan
    mine = lax.div(row, near)
    send(send_y, recv_y, 3, 3 + mine)
    recv_y[row] = send_y[row]

    def source(step):
        return wrapped(place + chips - step, chips)

    lower = wrapped(mine + GROUPS - 1, GROUPS)
    upper = wrapped(mine + 1, GROUPS)
    low_half = row - mine * near < near // 2
    groups = [mine, jnp.where(low_half, lower, upper), jnp.where(low_half, upper, lower)]

    def to_chip(at, step):
        return pltpu.make_async_remote_copy(
            src_ref=blocks.at[col, groups[at]],
            dst_ref=blocks.at[col, groups[at]],
            send_sem=near_send,
            recv_sem=near_recv.at[at, step],
            device_id=(row, wrapped(place + step, chips) * 2 + core),
            device_id_type=MESH,
        )

    def to_pair(at, step):
        own = source(step) * 2 + core
        return pltpu.make_async_remote_copy(
            src_ref=blocks.at[own, groups[at]],
            dst_ref=blocks.at[own, groups[at]],
            send_sem=pair_send,
            recv_sem=pair_recv.at[at, step],
            device_id=(row, partner),
            device_id_type=MESH,
        )

    def product(at, indices):
        left = jnp.concatenate([blocks[index, groups[at]] for index in indices], axis=0)
        starts = [pl.multiple_of(index * width + groups[at] * share, 16) for index in indices]
        right = jnp.concatenate([out_v[pl.ds(start, share), :] for start in starts], axis=0)
        return dot(left, right, ((0,), (0,)))

    steps = [chips // 2] + [s for d in range(chips // 2 - 1, 0, -1) for s in (d, chips - d)]
    far, close = steps[:3], steps[3:]
    for at in range(GROUPS):
        arrivals = recv_y.at[pl.ds(0, near - 1 if at == 0 else near)]
        group_in = pltpu.make_async_remote_copy(
            src_ref=arrivals,
            dst_ref=arrivals,
            send_sem=send_sem.at[3],
            recv_sem=recv_sem.at[3 + groups[at]],
            device_id=(wrapped(row + 1, rows), col),
            device_id_type=MESH,
        )
        timed(f"group_{at}_in", group_in.wait_recv)
        for r in range(near):
            spread[at, 4 * r : 4 * r + 4, :] = recv_y[groups[at] * near + r].astype(F32)
        for q in range(chan):
            plain[pl.ds(at * share + q, near, stride=chan), :] = spread[
                at, pl.ds(q, near, stride=4), :
            ]
        blocks[col, groups[at]] = plain[at * share : (at + 1) * share, :].astype(BF16)
        for step in far:
            to_chip(at, step).start()
        to_pair(at, 0).start()
    for at in range(GROUPS):
        for step in close:
            to_chip(at, step).start()
    timed("load_out", loads[13].wait)
    for parcel in range(3):
        all_of(outgoing[parcel], incoming[parcel], parcel).wait_send()
    timed("drain", all_of(send_y, recv_y, 3).wait_send)
    total = jnp.zeros((BLOCK, out_v.shape[1]), F32)
    def pass_on(at, some):
        for step in some:
            timed("near_in", to_chip(at, step).wait_recv)
            to_pair(at, step).start()

    for at in range(GROUPS - 1):
        pass_on(at, far[1:] + far[:1])
    for at in range(GROUPS):
        if at == GROUPS - 1:
            pass_on(at, far[1:] + far[:1])
        pass_on(at, close)
        if at > 0:
            for step in [0] + steps:
                timed("pair_in", to_pair(at - 1, step).wait_recv)
            total += product(at - 1, [source(step) * 2 + 1 - core for step in [0] + steps])
        total += product(at, [source(step) * 2 + core for step in [0] + steps])
    for step in [0] + steps:
        timed("pair_in", to_pair(GROUPS - 1, step).wait_recv)
    total += product(GROUPS - 1, [source(step) * 2 + 1 - core for step in [0] + steps])
    result[...] = total.astype(BF16)

    for sent, sem in ((steps, near_send), ([0] + steps, pair_send)):
        sent = blocks.at[pl.ds(0, len(sent))]
        pltpu.make_async_remote_copy(
            src_ref=sent,
            dst_ref=sent,
            send_sem=sem,
            recv_sem=recv_sem.at[0],
            device_id=(row, partner),
            device_id_type=MESH,
        ).wait_send()


def on_device(
    tokens,
    w_value,
    w_gate_one,
    w_gate_two,
    short_taps,
    filter_in,
    filter_mid,
    filter_out,
    decay_rate,
    skip,
    w_out,
):
    rows, cols = lax.axis_size("row"), lax.axis_size("col")
    width, depth = w_value.shape
    chan = width // rows
    seq_len = rows * BLOCK
    tables = [jnp.asarray(table) for table in constants(rows, seq_len)]
    vmem = pl.BlockSpec(memory_space=pltpu.VMEM)
    hbm = pl.BlockSpec(memory_space=pl.ANY)
    return pl.pallas_call(
        functools.partial(kernel, (rows, cols, chan)),
        out_shape=pltpu.VMEM((BLOCK, w_out.shape[1]), BF16),
        in_specs=[hbm] * 17,
        out_specs=vmem,
        scratch_shapes=[
            pltpu.SMEM(short_taps.shape, F32),
            pltpu.SMEM(skip.shape, F32),
            pltpu.SMEM(decay_rate.shape, F32),
            pltpu.VMEM(filter_in.shape, F32),
            pltpu.VMEM(filter_mid.shape, F32),
            pltpu.VMEM(filter_out.shape[:3] + (256,), F32),
            *[pltpu.VMEM(table.shape, table.dtype) for table in tables],
            pltpu.VMEM((256, 128), F32),
            pltpu.VMEM((BLOCK, depth), BF16),
            pltpu.VMEM((3, width, depth), BF16),
            pltpu.VMEM(w_out.shape, BF16),
            pltpu.VMEM((width, BLOCK), F32),
            pltpu.VMEM((3, 4 * rows, BLOCK), F32),
            pltpu.VMEM((16 * rows, BLOCK), F32),
            pltpu.VMEM((2, width, 2 * BLOCK), F32),
            *[pltpu.VMEM((rows, len(members), BLOCK), BF16) for members in PARCELS],
            *[pltpu.VMEM((rows, len(members), BLOCK), BF16) for members in PARCELS],
            pltpu.VMEM((rows, 4, BLOCK), BF16),
            pltpu.VMEM((rows, 4, BLOCK), BF16),
            pltpu.VMEM((cols, GROUPS, width // GROUPS, BLOCK), BF16),
            pltpu.SemaphoreType.DMA((17,)),
            pltpu.SemaphoreType.DMA((4,)),
            pltpu.SemaphoreType.DMA((3 + GROUPS,)),
            pltpu.SemaphoreType.DMA,
            pltpu.SemaphoreType.DMA((GROUPS, cols // 2)),
            pltpu.SemaphoreType.DMA,
            pltpu.SemaphoreType.DMA((GROUPS, cols // 2)),
        ],
        compiler_params=pltpu.CompilerParams(collective_id=0, has_side_effects=True),
    )(
        short_taps,
        skip,
        decay_rate,
        tokens,
        w_value,
        w_gate_one,
        w_gate_two,
        w_out,
        filter_in,
        filter_mid,
        filter_out,
        *tables,
    )


def solution(mesh):
    placed = (
        P("row", None),
        P("col", None),
        P("col", None),
        P("col", None),
        P(None, None, "col"),
        P(),
        P(),
        P(),
        P("col"),
        P(None, "col"),
        P(None, "col"),
    )
    return jax.shard_map(
        on_device, mesh=mesh, in_specs=placed, out_specs=P("row", "col"), check_vma=False
    )
```
